32 devices in a mesh: sp: 8 (over z, y), dp: 4 (over x, core).
Axes of the slice: x: 2, y: 2, z: 4, core: 2. Of those that a mesh axis runs over, the one named last changes fastest.
Arguments:
- residual: bfloat16 [4, 2048, 2048], P('dp', 'sp'), may hold values from -6 to 6
- queries: bfloat16 [4, 2048, 1024], P('dp', 'sp'), may hold values from -400 to 400
- key_vectors: bfloat16 [4, 2048, 1024], P('dp', 'sp'), may hold values from -6 to 6
- value_vectors: bfloat16 [4, 2048, 1024], P('dp', 'sp'), may hold values from -6 to 6
- gate_cache: float32 [4, 2048, 16], P('dp', 'sp'), may hold values from -258 to 0, as said below
- out_weight: bfloat16 [1024, 2048], P(None, 'dp'), may hold values from -0.1875 to 0.1875
- mix_gain: float32 [2048], replicated, may hold values from 0.1 to 1.9
- route_gain: float32 [2048], replicated, may hold values from 0.1 to 1.9
- out_gain: float32 [2048], replicated, may hold values from 0.1 to 1.9
- routes: int32 [4, 2048, 2], P('dp', 'sp'), may hold values from 0 to 7, all different within a row; in each aligned block of 256 rows (0 to 255, 256 to 511, ..., all dimensions but the last counted through in order) at most 128 rows name the same one
- group_share: float32 [4, 2048], P('dp', 'sp'), may hold values from 0.2 to 1
- expert_share: float32 [4, 2048, 2], P('dp', 'sp'), may hold values from 0.1 to 1
- gate_proj: bfloat16 [8, 2048, 1024], P('sp'), may hold values from -0.125 to 0.125
- up_proj: bfloat16 [8, 2048, 1024], P('sp'), may hold values from -0.125 to 0.125
- down_proj: bfloat16 [8, 1024, 2048], P('sp'), may hold values from -0.1875 to 0.1875
Outputs:
- layer_out: bfloat16 [4, 2048, 2048], P('dp', 'sp')
The draws below stay inside these ranges and needn't reach their ends.
Inputs may be any that keep to these rules, and one draw needn't show every extreme that they name: `gate_cache`: along the positions of a sequence the values never rise. `routes`: the 2 experts of a position differ. Within the rows of one device (aligned blocks of 256 positions) no expert is named more than 128 times, a bound that some block reaches.
All inputs are finite; a program needn't handle non-finite values.
Results may differ from the reference program's by a relative error of at most 0.0085.
Values may be sent and summed in bfloat16 or wider, within the bound.
A program may use at most 128 MiB of HBM per device.

```python
import math
import jax
import jax.numpy as jnp
import numpy as np
from jax import lax

D = 2048
HEADS = 16
FF = 1024
TOP = 2
TOK_DEV = 256
ATTN = 1024
SEQUENCE_LENGTH = 2048
SEQUENCE_COUNT = 4
EXPERTS = 8
CAP = 128


def drawn_pair(base):
    key_draw = jnp.clip(jax.random.normal(jax.random.fold_in(base, 11), (SEQUENCE_COUNT, SEQUENCE_LENGTH, ATTN), jnp.float32), -6.0, 6.0)
    query_draw = jnp.clip(jax.random.normal(jax.random.fold_in(base, 12), (SEQUENCE_COUNT, SEQUENCE_LENGTH, ATTN), jnp.float32), -6.0, 6.0)
    return (query_draw, key_draw)


def draw_queries(key, part):
    return drawn_pair(key)[0].astype(jnp.bfloat16)


def draw_key_vectors(key, part):
    return drawn_pair(key)[1].astype(jnp.bfloat16)


def draw_gate_cache(key, part):
    picks = jax.random.permutation(jax.random.fold_in(key, 21), HEADS)
    lagging_heads = (picks < HEADS // 2).astype(jnp.float32)
    fast_rate = jnp.exp(jax.random.uniform(jax.random.fold_in(key, 22), (HEADS,), jnp.float32, math.log(0.01), math.log(0.033)))
    decay_rate = lagging_heads * (0.6 / SEQUENCE_LENGTH) + (1.0 - lagging_heads) * fast_rate
    coarse_estimate = jax.random.uniform(jax.random.fold_in(key, 23), (SEQUENCE_COUNT, SEQUENCE_LENGTH, HEADS), jnp.float32, 0.3, 1.7)
    block_count = SEQUENCE_LENGTH // TOK_DEV
    multiplier = jnp.exp(jax.random.uniform(jax.random.fold_in(key, 24), (SEQUENCE_COUNT, block_count, 1, 1), jnp.float32, math.log(0.5), math.log(2.0)))
    multiplier = jnp.broadcast_to(multiplier, (SEQUENCE_COUNT, block_count, TOK_DEV, 1)).reshape(SEQUENCE_COUNT, SEQUENCE_LENGTH, 1)
    spike_position = jax.random.randint(jax.random.fold_in(key, 25), (SEQUENCE_COUNT, 1, 2), 1, SEQUENCE_LENGTH)
    spike_length = jax.random.uniform(jax.random.fold_in(key, 26), (SEQUENCE_COUNT, 1, 2), jnp.float32, 0.22, 0.69)
    token_position = jnp.arange(SEQUENCE_LENGTH)[None, :, None]
    spike_value = jnp.sum(jnp.where(token_position == spike_position, spike_length, 0.0), axis=2, keepdims=True)
    gate_logarithm = -decay_rate[None, None, :] * coarse_estimate * multiplier - spike_value * lagging_heads[None, None, :]
    return jnp.cumsum(gate_logarithm, axis=1).astype(jnp.float32)


def levels(stream_key, dims, pieces, smallest, high):
    level, own = 1.0, jax.random.fold_in(stream_key, 6)
    for axis_at, shards_of in pieces:
        steps = jnp.exp(jax.random.uniform(jax.random.fold_in(own, axis_at), (shards_of,), jnp.float32, smallest / len(pieces), high / len(pieces)))
        level = level * jnp.repeat(steps, dims[axis_at] // shards_of).reshape([-1 if axis == axis_at else 1 for axis in range(len(dims))])
    return level


def assign_block(stream_key, own, number, rows, amount, top, bound, slope):
    order = jax.random.permutation(stream_key, amount)
    packed, common = portions_of(amount, rows * top, bound, slope, True), portions_of(amount, rows * top, bound, slope, False)
    places = jnp.arange(amount)

    def named(sizes, offset_by):
        used = int((sizes > 0).sum())
        fixed = max(1, used // 4)
        passed = fixed + (places - fixed + offset_by * (used - fixed)) % max(1, amount - fixed)
        return jnp.zeros((amount,), jnp.int32).at[order[jnp.where(places < fixed, places, passed)]].set(jnp.asarray(sizes, jnp.int32))

    sizes = jnp.where(number % 4 == 0, named(packed, number // 4), named(common, number - number // 4 - 1))
    mixed = jax.random.permutation(jax.random.fold_in(own, 3), amount)
    donor, receiver = mixed[0:amount // 2 * 2:2], mixed[1:amount // 2 * 2:2]
    margin = jnp.minimum(sizes[donor] - 1, bound - sizes[receiver]) // 2
    margin = jnp.where((donor == order[0]) | (receiver == order[0]) | (sizes[receiver] == 0), 0, jnp.maximum(margin, 0))
    passed = jax.random.randint(jax.random.fold_in(own, 4), (amount // 2,), 0, 1 << 20) % (margin + 1)
    sizes = sizes.at[donor].add(-passed).at[receiver].add(passed)
    labels = jnp.searchsorted(jnp.cumsum(sizes), jnp.arange(rows * top), side="right").astype(jnp.int32)
    listing = labels.reshape(top, rows).T
    listing = listing[jax.random.permutation(jax.random.fold_in(own, 1), rows)]
    offset_by = jax.random.randint(jax.random.fold_in(own, 2), (rows, 1), 0, top)
    return jnp.take_along_axis(listing, (jnp.arange(top)[None, :] + offset_by) % top, axis=1)


def portions_of(amount, total, most, slope, full):
    loads = [(1 << 20) // math.isqrt(standing ** slope) + 1 for standing in range(1, amount + 1)]
    largest = most if full else min(most, max(-(-total // amount), total * loads[0] // sum(loads)))
    least = 1 if total - largest >= amount - 1 else 0
    given, rest = [largest] + [least] * (amount - 1), total - largest - least * (amount - 1)
    while rest > 0:
        movable = [i for i in range(1, amount) if given[i] < largest] or [i for i in range(1, amount) if given[i] < most]
        pool, remaining = sum([loads[i] for i in movable]), rest
        for i in movable:
            more = min(most - given[i], max(1, remaining * loads[i] // pool), rest)
            given[i] = given[i] + more
            rest = rest - more
    return np.array(given)


def bell_draw(stream_key, dims, spread, bound, cuts=(), held_as=jnp.bfloat16):
    loudness = levels(stream_key, dims, cuts, -0.22, 0.18) if cuts else 1.0
    values = jax.random.normal(stream_key, dims, jnp.float32) * spread * loudness
    return jnp.minimum(jnp.maximum(values, -bound), bound).astype(held_as)


def setup_inputs(seed: int = 0) -> dict:
    splits = jax.random.split(jax.random.key(seed), 16)
    residual = bell_draw(splits[0], (SEQUENCE_COUNT, SEQUENCE_LENGTH, D), 1.0, 6.0, ((0, 4), (1, 8)))
    queries = draw_queries(jax.random.fold_in(splits[15], 71), 0)
    key_vectors = draw_key_vectors(jax.random.fold_in(splits[15], 71), 0)
    value_vectors = bell_draw(splits[3], (SEQUENCE_COUNT, SEQUENCE_LENGTH, ATTN), 1.0, 6.0, ((0, 4), (1, 8)))
    gate_cache = draw_gate_cache(jax.random.fold_in(splits[15], 71), 0)
    out_weight = bell_draw(splits[5], (ATTN, D), ATTN ** -0.5, 0.1875, ((1, 4),))
    mix_gain = jnp.clip(1.0 + 0.18 * jax.random.normal(splits[6], (D,), jnp.float32), 0.1, 1.9)
    route_gain = jnp.clip(1.0 + 0.18 * jax.random.normal(splits[7], (D,), jnp.float32), 0.1, 1.9)
    out_gain = jnp.clip(1.0 + 0.18 * jax.random.normal(splits[8], (D,), jnp.float32), 0.1, 1.9)
    routes_keys = jax.random.split(jax.random.fold_in(splits[9], 1), SEQUENCE_COUNT * SEQUENCE_LENGTH // TOK_DEV)
    routes_turns = jax.random.permutation(jax.random.fold_in(splits[9], 3), SEQUENCE_COUNT * SEQUENCE_LENGTH // TOK_DEV)
    routes = jax.vmap(lambda own, number: assign_block(jax.random.fold_in(splits[9], 2), own, number, TOK_DEV, EXPERTS, TOP, CAP, 2))(routes_keys, routes_turns).reshape((SEQUENCE_COUNT, SEQUENCE_LENGTH, TOP))
    group_share = jnp.clip(jnp.exp(math.log(1.0) - 1.609438 * jax.random.uniform(splits[10], (SEQUENCE_COUNT, SEQUENCE_LENGTH), jnp.float32) ** levels(splits[10], (SEQUENCE_COUNT, SEQUENCE_LENGTH), ((0, 4), (1, 8)), -0.2, 0.2)), 0.2, 1.0)
    expert_share = jnp.clip(jnp.exp(math.log(1.0) - 2.3025851 * jax.random.uniform(splits[11], (SEQUENCE_COUNT, SEQUENCE_LENGTH, TOP), jnp.float32) ** levels(splits[11], (SEQUENCE_COUNT, SEQUENCE_LENGTH, TOP), ((0, 4), (1, 8)), -0.2, 0.2)), 0.1, 1.0)
    gate_proj = bell_draw(splits[12], (EXPERTS, D, FF), D ** -0.5, 0.125, ((0, 8),))
    up_proj = bell_draw(splits[13], (EXPERTS, D, FF), D ** -0.5, 0.125, ((0, 8),))
    down_proj = bell_draw(splits[14], (EXPERTS, FF, D), FF ** -0.5, 0.1875, ((0, 8),))
    return {"residual": residual, "queries": queries, "key_vectors": key_vectors, "value_vectors": value_vectors, "gate_cache": gate_cache, "out_weight": out_weight, "mix_gain": mix_gain, "route_gain": route_gain, "out_gain": out_gain, "routes": routes, "group_share": group_share, "expert_share": expert_share, "gate_proj": gate_proj, "up_proj": up_proj, "down_proj": down_proj}


def normalize(values):
    return values * lax.rsqrt(lax.optimization_barrier(jnp.mean(values * values, axis=-1, keepdims=True)) + 1e-06)

def attend(queries, key_vectors, value_vectors, cum_gates):
    length = queries.shape[0]
    head_count = cum_gates.shape[1]
    head_width = queries.shape[1] // head_count
    score_scale = head_width ** (-0.5)
    q_heads = queries.reshape(length, head_count, head_width).astype(jnp.float32)
    k_heads = key_vectors.reshape(length, head_count, head_width).astype(jnp.float32)
    v_heads = value_vectors.reshape(length, head_count, head_width).astype(jnp.float32)
    block_rows = min(512, length)
    outputs = []
    for offset in range(0, length, block_rows):
        stop = offset + block_rows
        scores = jnp.einsum('qhd,khd->hqk', q_heads[offset:stop], k_heads[:stop]) * score_scale
        bias = cum_gates[offset:stop].T[:, :, None] - cum_gates[:stop].T[:, None, :]
        row_pos = offset + jnp.arange(block_rows, dtype=jnp.int32)[:, None]
        col_pos = jnp.arange(stop, dtype=jnp.int32)[None, :]
        scores = jnp.where(col_pos <= row_pos, scores + bias, -1e+30)
        row_max = lax.optimization_barrier(jnp.max(scores, axis=-1, keepdims=True))
        expo_terms = jnp.exp(scores - row_max)
        probs = (expo_terms / lax.optimization_barrier(jnp.sum(expo_terms, axis=-1, keepdims=True))).astype(jnp.bfloat16)
        mixing = jnp.einsum('hqk,khd->qhd', probs.astype(jnp.float32), v_heads[:stop])
        outputs.append(mixing.astype(jnp.bfloat16).reshape(block_rows, head_count * head_width))
    return jnp.concatenate(outputs, axis=0)

def reference(residual, queries, key_vectors, value_vectors, gate_cache, out_weight, mix_gain, route_gain, out_gain, routes, group_share, expert_share, gate_proj, up_proj, down_proj):
    seq_count, length, model_width = residual.shape
    tokens = seq_count * length

    def one_sequence(operands):
        return attend(operands[0], operands[1], operands[2], operands[3])
    attended = lax.map(one_sequence, (queries, key_vectors, value_vectors, gate_cache))
    mixed = jnp.dot(attended.reshape(tokens, -1), out_weight, preferred_element_type=jnp.float32)
    hidden = (residual.reshape(tokens, model_width).astype(jnp.float32) + normalize(mixed) * mix_gain).astype(jnp.bfloat16)
    routed = (normalize(hidden.astype(jnp.float32)) * route_gain).astype(jnp.bfloat16)
    experts = gate_proj.shape[0]
    blocks = tokens // TOK_DEV
    count = TOK_DEV * TOP
    assigned = routes.reshape(blocks, count)
    expert_ids = jnp.arange(experts, dtype=jnp.int32)
    one_hot = (assigned[:, :, None] == expert_ids[None, None, :]).astype(jnp.int32)
    ranking = lax.optimization_barrier(jnp.sum((jnp.cumsum(one_hot, axis=1) - one_hot) * one_hot, axis=2))
    slot_index = assigned * CAP + ranking
    owners = jnp.broadcast_to(jnp.arange(count, dtype=jnp.int32)[None, :] // TOP, (blocks, count))
    block_ids = jnp.arange(blocks, dtype=jnp.int32)[:, None]
    shares = expert_share.reshape(tokens, TOP)
    weights = group_share.reshape(tokens, 1) * shares / lax.optimization_barrier(jnp.sum(shares, axis=1, keepdims=True))
    slot_token = jnp.full((blocks, experts * CAP), TOK_DEV, jnp.int32).at[block_ids, slot_index].set(owners)
    slot_weight = jnp.zeros((blocks, experts * CAP), jnp.float32).at[block_ids, slot_index].set(weights.reshape(blocks, count))
    padded = jnp.concatenate([routed.reshape(blocks, TOK_DEV, model_width), jnp.zeros((blocks, 1, model_width), jnp.bfloat16)], axis=1)

    def one_expert(totals, operands):
        w_gate, w_up, w_down, expert_index = operands
        tok_index = lax.dynamic_slice_in_dim(slot_token, expert_index * CAP, CAP, 1)
        w_slots = lax.dynamic_slice_in_dim(slot_weight, expert_index * CAP, CAP, 1)
        rows_in = padded[block_ids, tok_index].reshape(blocks * CAP, model_width)
        gate = jnp.dot(rows_in, w_gate, preferred_element_type=jnp.float32)
        upper = jnp.dot(rows_in, w_up, preferred_element_type=jnp.float32)
        act = (jax.nn.silu(gate) * upper).astype(jnp.bfloat16)
        result = jnp.dot(act, w_down, preferred_element_type=jnp.float32).astype(jnp.bfloat16)
        result = result.reshape(blocks, CAP, model_width).astype(jnp.float32)
        totals = totals.at[block_ids, tok_index].add(w_slots[:, :, None] * result)
        return (totals, None)
    start_totals = jnp.zeros((blocks, TOK_DEV + 1, model_width), jnp.float32)
    totals, unused = lax.scan(one_expert, start_totals, (gate_proj, up_proj, down_proj, jnp.arange(experts, dtype=jnp.int32)))
    combined = totals[:, :TOK_DEV].reshape(tokens, model_width)
    layer_out = (hidden.astype(jnp.float32) + combined * out_gain).astype(jnp.bfloat16)
    return layer_out.reshape(seq_count, length, model_width)
```

```python
import functools
import math
import jax
import jax.numpy as jnp
from jax import lax
from jax.experimental import pallas as pl
from jax.experimental.pallas import tpu as pltpu
from jax.sharding import PartitionSpec as P

LOG2E = math.log2(math.e)
MESH = pl.DeviceIdType.MESH


def normalize(values):
    return values * lax.rsqrt(jnp.mean(values * values, axis=-1, keepdims=True) + 1e-06)


def attend(queries, key_rows, value_rows, cum_gates):
    length = queries.shape[0]
    head_count = cum_gates.shape[1]
    head_width = queries.shape[1] // head_count
    score_scale = head_width ** (-0.5)
    q_heads = queries.reshape(length, head_count, head_width)
    k_heads = key_rows.reshape(length, head_count, head_width)
    v_heads = value_rows.reshape(length, head_count, head_width)
    block_rows = min(512, length)
    outputs = []
    for offset in range(0, length, block_rows):
        stop = offset + block_rows
        scores = (
            jnp.einsum(
                "qhd,khd->hqk",
                q_heads[offset:stop],
                k_heads[:stop],
                preferred_element_type=jnp.float32,
            )
            * score_scale
        )
        bias = cum_gates[offset:stop].T[:, :, None] - cum_gates[:stop].T[:, None, :]
        row_pos = offset + jnp.arange(block_rows, dtype=jnp.int32)[:, None]
        col_pos = jnp.arange(stop, dtype=jnp.int32)[None, :]
        scores = jnp.where(col_pos <= row_pos, scores + bias, -1e30)
        row_max = jnp.max(scores, axis=-1, keepdims=True)
        expo_terms = jnp.exp(scores - row_max)
        probs = (expo_terms / jnp.sum(expo_terms, axis=-1, keepdims=True)).astype(jnp.bfloat16)
        mixing = jnp.einsum(
            "hqk,khd->qhd", probs, v_heads[:stop], preferred_element_type=jnp.float32
        )
        outputs.append(mixing.astype(jnp.bfloat16).reshape(block_rows, head_count * head_width))
    return jnp.concatenate(outputs, axis=0)

def mix_kernel(
    block, heads, span, spread,
    q_in, k_in, v_in, g_in, ow_in, tok_out, ow_out,
    q_all, k_all, v_all, g_all, att, send, recv, back_send, back_recv, ow_send, ow_recv,
):
    me = lax.axis_index("sp")
    mine = lax.axis_index("dp")
    rows = q_in.shape[0]
    width = q_all.shape[1]
    cols = ow_in.shape[1]
    barrier = pltpu.get_barrier_semaphore()
    for d in range(1, span):
        pl.semaphore_signal(barrier, inc=1, device_id={"sp": lax.rem(me + d, span)}, device_id_type=MESH)
    for d in range(1, spread):
        pl.semaphore_signal(barrier, inc=1, device_id={"dp": lax.rem(mine + d, spread)}, device_id_type=MESH)
    pl.semaphore_wait(barrier, span + spread - 2)

    own_rows = pl.ds(pl.multiple_of(me * rows, rows), rows)
    pairs = ((q_in, q_all), (k_in, k_all), (v_in, v_all))
    sends = []
    for d in sorted(range(1, span), key=lambda d: -min(d, span - d)):
        peer = lax.rem(me + d, span)
        lanes = pl.ds(pl.multiple_of(peer * width, width), width)
        for a, (src, dst) in enumerate(pairs):
            sends.append(
                pltpu.make_async_remote_copy(
                    src_ref=src.at[:, lanes], dst_ref=dst.at[own_rows, :],
                    send_sem=send.at[a, d], recv_sem=recv.at[a, me],
                    device_id={"sp": peer}, device_id_type=MESH,
                )
            )
        sends.append(
            pltpu.make_async_remote_copy(
                src_ref=g_in.at[peer], dst_ref=g_all.at[me],
                send_sem=send.at[3, d], recv_sem=recv.at[3, me],
                device_id={"sp": peer}, device_id_type=MESH,
            )
        )
    ow_lanes = pl.ds(pl.multiple_of(mine * cols, cols), cols)
    ow_sends = []
    for d in range(1, spread):
        ow_sends.append(
            pltpu.make_async_remote_copy(
                src_ref=ow_in, dst_ref=ow_out.at[:, ow_lanes],
                send_sem=ow_send.at[d], recv_sem=ow_recv.at[d],
                device_id={"dp": lax.rem(mine + d, spread)}, device_id_type=MESH,
            )
        )
    for copy in sends + ow_sends:
        copy.start()
    own_lanes = pl.ds(pl.multiple_of(me * width, width), width)
    for a, (src, dst) in enumerate(pairs):
        pltpu.make_async_copy(src.at[:, own_lanes], dst.at[own_rows, :], recv.at[a, me]).start()
    pltpu.make_async_copy(g_in.at[me], g_all.at[me], recv.at[3, me]).start()
    ow_local = pltpu.make_async_copy(ow_in, ow_out.at[:, ow_lanes], ow_recv.at[0])
    ow_local.start()

    scale = (width // heads) ** -0.5 * LOG2E
    lane = lax.broadcasted_iota(jnp.int32, (1, width), 1)
    in_head = [(lane // (width // heads)) == h for h in range(heads)]
    row = lax.broadcasted_iota(jnp.int32, (block, block), 0)
    col = lax.broadcasted_iota(jnp.int32, (block, block), 1)
    keep = col <= row
    ones = jnp.ones((block, width), jnp.bfloat16)
    per = block // rows

    def arrive(s):
        at = pl.ds(s * rows, rows)
        for a, (_, dst) in enumerate(pairs):
            pltpu.make_async_copy(dst.at[at, :], dst.at[at, :], recv.at[a, s]).wait()
        pltpu.make_async_copy(g_all.at[s], g_all.at[s], recv.at[3, s]).wait()

    def returned(s):
        return pltpu.make_async_remote_copy(
            src_ref=att.at[pl.ds(s * rows, rows), :], dst_ref=tok_out.at[:, own_lanes],
            send_sem=back_send.at[s], recv_sem=back_recv.at[me],
            device_id={"sp": s}, device_id_type=MESH,
        )

    for i in range(span // per):
        for s in range(i * per, (i + 1) * per):
            arrive(s)
        q = q_all[pl.ds(i * block, block), :]
        outs = []
        for h in range(heads):
            qh = jnp.where(in_head[h], q, jnp.zeros_like(q))
            scores = []
            top = None
            for j in range(i + 1):
                s = lax.dot_general(
                    qh, k_all[pl.ds(j * block, block), :], (((1,), (1,)), ((), ())),
                    preferred_element_type=jnp.float32,
                )
                gate = jnp.concatenate(
                    [g_all[j * per + t, pl.ds(h, 1), :] for t in range(per)], axis=1
                )
                s = s * scale - gate * LOG2E
                if j == i:
                    s = jnp.where(keep, s, -1e30)
                scores.append(s)
                peak = jnp.max(s, axis=1, keepdims=True)
                top = peak if top is None else jnp.maximum(top, peak)
            acc = None
            for j in range(i + 1):
                p = jnp.exp2(scores[j] - top).astype(jnp.bfloat16)
                rhs = jnp.concatenate([v_all[pl.ds(j * block, block), :], ones], axis=1)
                part = jnp.dot(p, rhs, preferred_element_type=jnp.float32)
                acc = part if acc is None else acc + part
            outs.append(acc[:, :width] / acc[:, width:])
        out = outs[0]
        for h in range(1, heads):
            out = jnp.where(in_head[h], outs[h], out)
        att[pl.ds(i * block, block), :] = out.astype(att.dtype)
        for s in range(i * per, (i + 1) * per):
            @pl.when(me != s)
            def _():
                returned(s).start()

            @pl.when(me == s)
            def _():
                pltpu.make_async_copy(
                    att.at[pl.ds(s * rows, rows), :], tok_out.at[:, own_lanes], back_recv.at[s]
                ).start()
    for s in range(span):
        at = pl.ds(s * width, width)
        pltpu.make_async_copy(tok_out.at[:, at], tok_out.at[:, at], back_recv.at[s]).wait()

        @pl.when(me != s)
        def _():
            returned(s).wait_send()
    for copy in sends:
        copy.wait_send()
    ow_local.wait()
    for copy in ow_sends:
        copy.wait()


def mix(queries, keys, values, gates, out_weight, span, spread):
    rows, full = queries.shape
    width = full // span
    heads = gates.shape[1] // span
    per = 2 if span % 2 == 0 else 1
    g = gates.T.reshape(span, heads, rows)
    vm = pl.BlockSpec(memory_space=pltpu.VMEM)
    dma = pltpu.SemaphoreType.DMA
    wide = pltpu.VMEM((span * rows, width), jnp.bfloat16)
    return pl.pallas_call(
        functools.partial(mix_kernel, per * rows, heads, span, spread),
        out_shape=(
            jax.ShapeDtypeStruct((rows, full), jnp.bfloat16),
            jax.ShapeDtypeStruct((full, out_weight.shape[1] * spread), jnp.bfloat16),
        ),
        in_specs=[vm] * 5,
        out_specs=(vm, vm),
        scratch_shapes=[
            wide, wide, wide, pltpu.VMEM((span, heads, rows), jnp.float32), wide,
            dma((4, span)), dma((4, span)), dma((span,)), dma((span,)), dma((spread,)), dma((spread,)),
        ],
        compiler_params=pltpu.CompilerParams(
            collective_id=0, has_side_effects=True, vmem_limit_bytes=50 * 1024 * 1024
        ),
        name="mix",
    )(queries, keys, values, g, out_weight)


def experts_kernel(
    span, chunks,
    routed, pick, weigh, gate_in, up_in, down_in, out,
    w_gate, w_up, w_down, mir, out_own, out_mir, arrived, act, res, back, pbuf, part,
    w_sem, mir_s, mir_r, dir_s, dir_r, two_s, two_r, ret_s, ret_r, rt1_s, rt1_r, part_s, part_r,
):
    half = span // 2
    me = lax.axis_index("sp")
    base = (me // half) * half
    loc = me - base
    mirror = lax.rem(me + half, span)
    cap = arrived.shape[2]
    model = routed.shape[1]
    piece = model // chunks
    ff = act.shape[1]
    partners = [(d, lax.rem(loc + d, half)) for d in range(1, half)]
    barrier = pltpu.get_barrier_semaphore()
    for _, p in partners:
        pl.semaphore_signal(barrier, inc=1, device_id={"sp": base + p}, device_id_type=MESH)
    pl.semaphore_signal(barrier, inc=1, device_id={"sp": mirror}, device_id_type=MESH)
    pl.semaphore_wait(barrier, half)

    def remote(src, dst, s_sem, r_sem, device):
        return pltpu.make_async_remote_copy(
            src_ref=src, dst_ref=dst, send_sem=s_sem, recv_sem=r_sem,
            device_id={"sp": device}, device_id_type=MESH,
        )

    def cols(c):
        return pl.ds(c * piece, piece)

    pending = []

    def begin(copy):
        copy.start()
        pending.append(copy)

    for c in range(chunks):
        begin(remote(routed.at[:, cols(c)], mir.at[:, cols(c)], mir_s.at[c], mir_r.at[c], mirror))
    loads = [
        pltpu.make_async_copy(src, dst, w_sem.at[i])
        for i, (src, dst) in enumerate(((gate_in, w_gate), (up_in, w_up), (down_in, w_down)))
    ]
    for load in loads:
        load.start()

    def rows_of(p):
        return pl.ds(pl.multiple_of(p * cap, cap), cap)

    for d, p in partners:
        chosen = pick[0, rows_of(p), :]
        for c in range(chunks):
            out_own[p, :, cols(c)] = jnp.dot(
                chosen, routed[:, cols(c)], preferred_element_type=jnp.float32
            ).astype(jnp.bfloat16)
        begin(remote(out_own.at[p], arrived.at[0, loc], dir_s.at[d], dir_r.at[loc], base + p))
    chosen = pick[0, rows_of(loc), :]
    for c in range(chunks):
        arrived[0, loc, :, cols(c)] = jnp.dot(
            chosen, routed[:, cols(c)], preferred_element_type=jnp.float32
        ).astype(jnp.bfloat16)

    for c in range(chunks):
        remote(mir.at[:, cols(c)], mir.at[:, cols(c)], mir_s.at[c], mir_r.at[c], mirror).wait_recv()
        for d, p in partners:
            out_mir[p, :, cols(c)] = jnp.dot(
                pick[1, rows_of(p), :], mir[:, cols(c)], preferred_element_type=jnp.float32
            ).astype(jnp.bfloat16)
            begin(
                remote(
                    out_mir.at[p, :, cols(c)], arrived.at[1, loc, :, cols(c)],
                    two_s.at[d, c], two_r.at[loc, c], base + p,
                )
            )
        arrived[1, loc, :, cols(c)] = jnp.dot(
            pick[1, rows_of(loc), :], mir[:, cols(c)], preferred_element_type=jnp.float32
        ).astype(jnp.bfloat16)

    for load in loads:
        load.wait()

    def hidden_units(g):
        tile = math.gcd(256, ff)
        rows_in = arrived.at[g]

        def step(f, carry):
            at = pl.ds(pl.multiple_of(f * tile, tile), tile)
            data = rows_in[...].reshape(half * cap, model)
            gate = jnp.dot(data, w_gate[:, at], preferred_element_type=jnp.float32)
            upper = jnp.dot(data, w_up[:, at], preferred_element_type=jnp.float32)
            act[:, at] = (gate / (1.0 + jnp.exp(-gate)) * upper).astype(jnp.bfloat16)
            return carry

        lax.fori_loop(0, ff // tile, step, 0)

    def results(g, c):
        value = jnp.dot(act[...], w_down[:, cols(c)], preferred_element_type=jnp.float32)
        res[g, :, :, cols(c)] = value.astype(jnp.bfloat16).reshape(half, cap, piece)

    def total(g, c):
        data = back[g, :, :, cols(c)].reshape(half * cap, piece)
        high = jnp.dot(weigh[g, 0], data, preferred_element_type=jnp.float32)
        return high + jnp.dot(weigh[g, 1], data, preferred_element_type=jnp.float32)

    for d, p in partners:
        remote(out_own.at[p], arrived.at[0, p], dir_s.at[d], dir_r.at[p], base + p).wait_recv()
    hidden_units(0)
    for c in range(chunks):
        results(0, c)
    for d, p in partners:
        begin(remote(res.at[0, p], back.at[0, loc], ret_s.at[d], ret_r.at[loc], base + p))
    back[0, loc] = res[0, loc]

    for c in range(chunks):
        for d, p in partners:
            remote(
                out_mir.at[p, :, cols(c)], arrived.at[1, p, :, cols(c)],
                two_s.at[d, c], two_r.at[p, c], base + p,
            ).wait_recv()
    hidden_units(1)
    for c in range(chunks):
        results(1, c)
        for d, p in partners:
            begin(
                remote(
                    res.at[1, p, :, cols(c)], back.at[1, loc, :, cols(c)],
                    rt1_s.at[d, c], rt1_r.at[loc, c], base + p,
                )
            )
        back[1, loc, :, cols(c)] = res[1, loc, :, cols(c)]
    for c in range(chunks):
        for d, p in partners:
            remote(
                res.at[1, p, :, cols(c)], back.at[1, p, :, cols(c)],
                rt1_s.at[d, c], rt1_r.at[p, c], base + p,
            ).wait_recv()
        pbuf[:, cols(c)] = total(1, c).astype(jnp.bfloat16)
        begin(remote(pbuf.at[:, cols(c)], part.at[:, cols(c)], part_s.at[c], part_r.at[c], mirror))
    for d, p in partners:
        remote(res.at[0, p], back.at[0, p], ret_s.at[d], ret_r.at[p], base + p).wait_recv()
    for c in range(chunks):
        own = total(0, c)
        remote(pbuf.at[:, cols(c)], part.at[:, cols(c)], part_s.at[c], part_r.at[c], mirror).wait_recv()
        out[:, cols(c)] = own + part[:, cols(c)].astype(jnp.float32)
    for copy in pending:
        copy.wait_send()


def run_experts(routed, pick, weigh, gate_proj, up_proj, down_proj, span, cap):
    rows, model = routed.shape
    ff = gate_proj.shape[1]
    half = span // 2
    chunks = 4 if model % 512 == 0 else 1
    vm = pl.BlockSpec(memory_space=pltpu.VMEM)
    hbm = pl.BlockSpec(memory_space=pl.ANY)
    dma = pltpu.SemaphoreType.DMA
    bf16 = jnp.bfloat16
    return pl.pallas_call(
        functools.partial(experts_kernel, span, chunks),
        out_shape=jax.ShapeDtypeStruct((rows, model), jnp.float32),
        in_specs=[vm, vm, vm, hbm, hbm, hbm],
        out_specs=vm,
        scratch_shapes=[
            pltpu.VMEM((model, ff), bf16), pltpu.VMEM((model, ff), bf16), pltpu.VMEM((ff, model), bf16),
            pltpu.VMEM((rows, model), bf16),
            pltpu.VMEM((half, cap, model), bf16), pltpu.VMEM((half, cap, model), bf16),
            pltpu.VMEM((2, half, cap, model), bf16),
            pltpu.VMEM((half * cap, ff), bf16),
            pltpu.VMEM((2, half, cap, model), bf16), pltpu.VMEM((2, half, cap, model), bf16),
            pltpu.VMEM((rows, model), bf16), pltpu.VMEM((rows, model), bf16),
            dma((3,)), dma((chunks,)), dma((chunks,)), dma((half,)), dma((half,)),
            dma((half, chunks)), dma((half, chunks)), dma((half,)), dma((half,)),
            dma((half, chunks)), dma((half, chunks)), dma((chunks,)), dma((chunks,)),
        ],
        compiler_params=pltpu.CompilerParams(
            collective_id=1, has_side_effects=True, vmem_limit_bytes=58 * 1024 * 1024
        ),
        name="experts",
    )(routed, pick, weigh, gate_proj, up_proj, down_proj)


def body(
    residual, queries, key_vectors, value_vectors, gate_cache, out_weight, mix_gain, route_gain,
    out_gain, routes, group_share, expert_share, gate_proj, up_proj, down_proj,
):
    span = lax.axis_size("sp")
    spread = lax.axis_size("dp")
    tok_rows = residual.shape[1]
    width = queries.shape[2] // span

    cap = 4 * tok_rows // span
    half = span // 2
    assigned = routes[0].reshape(-1)
    order = jnp.arange(assigned.shape[0], dtype=jnp.int32)
    same = (assigned[:, None] == assigned[None, :]) & (order[None, :] < order[:, None])
    ranking = jnp.sum(same.astype(jnp.int32), axis=1)
    slots = (assigned * cap + ranking).reshape(routes.shape[1:]).astype(jnp.float32)
    shares = expert_share[0]
    weights = group_share[0][:, None] * shares / jnp.sum(shares, axis=1, keepdims=True)
    facts = jnp.stack([slots, weights])
    other = lax.ppermute(facts, "sp", [(i, (i + half) % span) for i in range(span)])
    base = (lax.axis_index("sp") // half) * half
    places = (base * cap + jnp.arange(half * cap, dtype=jnp.int32)).astype(jnp.float32)
    picks, weighs = [], []
    for both in (facts, other):
        hit = both[0][:, :, None] == places[None, None, :]
        picks.append(jnp.any(hit, axis=1).T.astype(jnp.bfloat16))
        high = lax.reduce_precision(both[1], 8, 7)
        weighs.append(
            jnp.stack(
                [jnp.sum(jnp.where(hit, w[:, :, None], 0.0), axis=1) for w in (high, both[1] - high)]
            ).astype(jnp.bfloat16)
        )
    pick, weigh = jnp.stack(picks), jnp.stack(weighs)

    if width % 128 == 0:
        by_tokens, weight_all = mix(
            queries[0], key_vectors[0], value_vectors[0], gate_cache[0], out_weight, span, spread
        )
    else:
        by_heads = [
            lax.all_to_all(x, "sp", split_axis=2, concat_axis=1, tiled=True)
            for x in (queries, key_vectors, value_vectors, gate_cache)
        ]
        attended = attend(*(x[0] for x in by_heads))
        by_tokens = lax.all_to_all(attended[None], "sp", split_axis=1, concat_axis=2, tiled=True)[0]
        weight_all = lax.all_gather(out_weight, "dp", axis=1, tiled=True)
    mixed = jnp.dot(by_tokens, weight_all, preferred_element_type=jnp.float32)
    hidden = (residual[0].astype(jnp.float32) + normalize(mixed) * mix_gain).astype(jnp.bfloat16)
    routed = (normalize(hidden.astype(jnp.float32)) * route_gain).astype(jnp.bfloat16)
    combined = run_experts(routed, pick, weigh, gate_proj[0], up_proj[0], down_proj[0], span, cap)
    layer_out = (hidden.astype(jnp.float32) + combined * out_gain).astype(jnp.bfloat16)
    return layer_out[None]


def solution(mesh):
    placed = (
        P("dp", "sp", None),
        P("dp", "sp", None),
        P("dp", "sp", None),
        P("dp", "sp", None),
        P("dp", "sp", None),
        P(None, "dp"),
        P(),
        P(),
        P(),
        P("dp", "sp", None),
        P("dp", "sp"),
        P("dp", "sp", None),
        P("sp", None, None),
        P("sp", None, None),
        P("sp", None, None),
    )
    return jax.shard_map(
        body, mesh=mesh, in_specs=placed, out_specs=P("dp", "sp", None), check_vma=False
    )
```

```python
import functools
import math
import jax
import jax.numpy as jnp
from jax import lax
from jax.experimental import pallas as pl
from jax.experimental.pallas import tpu as pltpu
from jax.sharding import PartitionSpec as P

LOG2E = math.log2(math.e)
MESH = pl.DeviceIdType.MESH


def normalize(values):
    return values * lax.rsqrt(jnp.mean(values * values, axis=-1, keepdims=True) + 1e-06)


def attend(queries, key_rows, value_rows, cum_gates):
    length = queries.shape[0]
    head_count = cum_gates.shape[1]
    head_width = queries.shape[1] // head_count
    score_scale = head_width ** (-0.5)
    q_heads = queries.reshape(length, head_count, head_width)
    k_heads = key_rows.reshape(length, head_count, head_width)
    v_heads = value_rows.reshape(length, head_count, head_width)
    block_rows = min(512, length)
    outputs = []
    for offset in range(0, length, block_rows):
        stop = offset + block_rows
        scores = (
            jnp.einsum(
                "qhd,khd->hqk",
                q_heads[offset:stop],
                k_heads[:stop],
                preferred_element_type=jnp.float32,
            )
            * score_scale
        )
        bias = cum_gates[offset:stop].T[:, :, None] - cum_gates[:stop].T[:, None, :]
        row_pos = offset + jnp.arange(block_rows, dtype=jnp.int32)[:, None]
        col_pos = jnp.arange(stop, dtype=jnp.int32)[None, :]
        scores = jnp.where(col_pos <= row_pos, scores + bias, -1e30)
        row_max = jnp.max(scores, axis=-1, keepdims=True)
        expo_terms = jnp.exp(scores - row_max)
        probs = (expo_terms / jnp.sum(expo_terms, axis=-1, keepdims=True)).astype(jnp.bfloat16)
        mixing = jnp.einsum(
            "hqk,khd->qhd", probs, v_heads[:stop], preferred_element_type=jnp.float32
        )
        outputs.append(mixing.astype(jnp.bfloat16).reshape(block_rows, head_count * head_width))
    return jnp.concatenate(outputs, axis=0)

def is_edge(me, loc, half):
    lower = me < half
    first = loc < half // 2
    return jnp.logical_or(
        jnp.logical_and(lower, first),
        jnp.logical_and(jnp.logical_not(lower), jnp.logical_not(first)),
    )


def mix_kernel(
    block, heads, span, spread,
    q_in, k_in, v_in, g_in, ow_in, facts, residual, gains, hidden_out, routed_out, others,
    tok_out, ow_out, mixed, fact_sem, q_all, k_all, v_all, g_all, att, send, recv, back_send, back_recv, ow_send, ow_recv,
):
    me = lax.axis_index("sp")
    mine = lax.axis_index("dp")
    rows = q_in.shape[0]
    width = q_all.shape[1]
    cols = ow_in.shape[1]
    barrier = pltpu.get_barrier_semaphore()
    for d in range(1, span):
        pl.semaphore_signal(barrier, inc=1, device_id={"sp": lax.rem(me + d, span)}, device_id_type=MESH)
    for d in range(1, spread):
        pl.semaphore_signal(barrier, inc=1, device_id={"dp": lax.rem(mine + d, spread)}, device_id_type=MESH)
    pl.semaphore_wait(barrier, span + spread - 2)

    own_rows = pl.ds(pl.multiple_of(me * rows, rows), rows)
    pairs = ((q_in, q_all), (k_in, k_all), (v_in, v_all))
    half = span // 2
    base = (me // half) * half
    loc = me - base
    mirror = lax.rem(me + half, span)
    fact_send = pltpu.make_async_remote_copy(
        src_ref=facts, dst_ref=others, send_sem=fact_sem.at[0], recv_sem=fact_sem.at[1],
        device_id={"sp": mirror}, device_id_type=MESH,
    )
    fact_send.start()

    def to_peer(d, peer):
        lanes = pl.ds(pl.multiple_of(peer * width, width), width)
        copies = [
            pltpu.make_async_remote_copy(
                src_ref=src.at[:, lanes], dst_ref=dst.at[own_rows, :],
                send_sem=send.at[a, d], recv_sem=recv.at[a, me],
                device_id={"sp": peer}, device_id_type=MESH,
            )
            for a, (src, dst) in enumerate(pairs)
        ]
        copies.append(
            pltpu.make_async_remote_copy(
                src_ref=g_in.at[peer], dst_ref=g_all.at[me],
                send_sem=send.at[3, d], recv_sem=recv.at[3, me],
                device_id={"sp": peer}, device_id_type=MESH,
            )
        )
        return copies

    near = [copy for d in range(1, half) for copy in to_peer(d, base + lax.rem(loc + d, half))]
    far = [
        copy
        for d in range(half)
        for copy in to_peer(half + d, (half - base) + lax.rem(loc + d, half))
    ]
    edge = is_edge(me, loc, half)

    @pl.when(edge)
    def _():
        for copy in near + far:
            copy.start()

    @pl.when(jnp.logical_not(edge))
    def _():
        for copy in far + near:
            copy.start()

    sends = near + far
    ow_lanes = pl.ds(pl.multiple_of(mine * cols, cols), cols)
    ow_sends = []
    for d in range(1, spread):
        ow_sends.append(
            pltpu.make_async_remote_copy(
                src_ref=ow_in, dst_ref=ow_out.at[:, ow_lanes],
                send_sem=ow_send.at[d], recv_sem=ow_recv.at[d],
                device_id={"dp": lax.rem(mine + d, spread)}, device_id_type=MESH,
            )
        )
    for copy in ow_sends:
        copy.start()
    own_lanes = pl.ds(pl.multiple_of(me * width, width), width)
    for a, (src, dst) in enumerate(pairs):
        pltpu.make_async_copy(src.at[:, own_lanes], dst.at[own_rows, :], recv.at[a, me]).start()
    pltpu.make_async_copy(g_in.at[me], g_all.at[me], recv.at[3, me]).start()
    ow_local = pltpu.make_async_copy(ow_in, ow_out.at[:, ow_lanes], ow_recv.at[0])
    ow_local.start()

    scale = (width // heads) ** -0.5 * LOG2E
    lane = lax.broadcasted_iota(jnp.int32, (1, width), 1)
    in_head = [(lane // (width // heads)) == h for h in range(heads)]
    row = lax.broadcasted_iota(jnp.int32, (block, block), 0)
    col = lax.broadcasted_iota(jnp.int32, (block, block), 1)
    keep = col <= row
    ones = jnp.ones((block, width), jnp.bfloat16)
    per = block // rows

    def arrive(s):
        at = pl.ds(s * rows, rows)
        for a, (_, dst) in enumerate(pairs):
            pltpu.make_async_copy(dst.at[at, :], dst.at[at, :], recv.at[a, s]).wait()
        pltpu.make_async_copy(g_all.at[s], g_all.at[s], recv.at[3, s]).wait()

    def returned(s):
        return pltpu.make_async_remote_copy(
            src_ref=att.at[pl.ds(s * rows, rows), :], dst_ref=tok_out.at[:, own_lanes],
            send_sem=back_send.at[s], recv_sem=back_recv.at[me],
            device_id={"sp": s}, device_id_type=MESH,
        )

    for i in range(span // per):
        for s in range(i * per, (i + 1) * per):
            arrive(s)
        q = q_all[pl.ds(i * block, block), :]
        outs = []
        for h in range(heads):
            qh = jnp.where(in_head[h], q, jnp.zeros_like(q))
            scores = []
            top = None
            for j in range(i + 1):
                s = lax.dot_general(
                    qh, k_all[pl.ds(j * block, block), :], (((1,), (1,)), ((), ())),
                    preferred_element_type=jnp.float32,
                )
                gate = jnp.concatenate(
                    [g_all[j * per + t, pl.ds(h, 1), :] for t in range(per)], axis=1
                )
                s = s * scale - gate * LOG2E
                if j == i:
                    s = jnp.where(keep, s, -1e30)
                scores.append(s)
                peak = jnp.max(s, axis=1, keepdims=True)
                top = peak if top is None else jnp.maximum(top, peak)
            acc = None
            for j in range(i + 1):
                p = jnp.exp2(scores[j] - top).astype(jnp.bfloat16)
                rhs = jnp.concatenate([v_all[pl.ds(j * block, block), :], ones], axis=1)
                part = jnp.dot(p, rhs, preferred_element_type=jnp.float32)
                acc = part if acc is None else acc + part
            outs.append(acc[:, :width] / acc[:, width:])
        out = outs[0]
        for h in range(1, heads):
            out = jnp.where(in_head[h], outs[h], out)
        att[pl.ds(i * block, block), :] = out.astype(att.dtype)
        for s in range(i * per, (i + 1) * per):
            @pl.when(me != s)
            def _():
                returned(s).start()

            @pl.when(me == s)
            def _():
                pltpu.make_async_copy(
                    att.at[pl.ds(s * rows, rows), :], tok_out.at[:, own_lanes], back_recv.at[s]
                ).start()
    for s in range(span):
        at = pl.ds(s * width, width)
        pltpu.make_async_copy(tok_out.at[:, at], tok_out.at[:, at], back_recv.at[s]).wait()

        @pl.when(me != s)
        def _():
            returned(s).wait_send()
    ow_local.wait()
    for copy in ow_sends:
        copy.wait()
    model = mixed.shape[1]
    piece = math.gcd(512, model)
    square = jnp.zeros((rows, 1), jnp.float32)
    for c in range(model // piece):
        value = jnp.dot(
            tok_out[...], ow_out[:, pl.ds(c * piece, piece)], preferred_element_type=jnp.float32
        )
        mixed[:, pl.ds(c * piece, piece)] = value
        square = square + jnp.sum(value * value, axis=1, keepdims=True)
    inverse = lax.rsqrt(square / model + 1e-06)
    square = jnp.zeros((rows, 1), jnp.float32)
    for c in range(model // piece):
        at = pl.ds(c * piece, piece)
        value = residual[:, at].astype(jnp.float32) + mixed[:, at] * inverse * gains[pl.ds(0, 1), at]
        value = value.astype(jnp.bfloat16)
        hidden_out[:, at] = value
        value = value.astype(jnp.float32)
        square = square + jnp.sum(value * value, axis=1, keepdims=True)
    inverse = lax.rsqrt(square / model + 1e-06)
    for c in range(model // piece):
        at = pl.ds(c * piece, piece)
        value = hidden_out[:, at].astype(jnp.float32) * inverse * gains[pl.ds(1, 1), at]
        routed_out[:, at] = value.astype(jnp.bfloat16)
    fact_send.wait()
    for copy in sends:
        copy.wait_send()


def mix(queries, keys, values, gates, out_weight, facts, residual, gains, span, spread):
    rows, full = queries.shape
    width = full // span
    heads = gates.shape[1] // span
    per = 2 if span % 2 == 0 else 1
    g = gates.T.reshape(span, heads, rows)
    vm = pl.BlockSpec(memory_space=pltpu.VMEM)
    hbm = pl.BlockSpec(memory_space=pl.ANY)
    dma = pltpu.SemaphoreType.DMA
    wide = pltpu.VMEM((span * rows, width), jnp.bfloat16)
    return pl.pallas_call(
        functools.partial(mix_kernel, per * rows, heads, span, spread),
        out_shape=(
            jax.ShapeDtypeStruct(residual.shape, jnp.bfloat16),
            jax.ShapeDtypeStruct(residual.shape, jnp.bfloat16),
            jax.ShapeDtypeStruct(facts.shape, jnp.float32),
        ),
        in_specs=[hbm, hbm, hbm, vm, hbm, vm, vm, vm],
        out_specs=(vm, vm, vm),
        scratch_shapes=[
            pltpu.VMEM((rows, full), jnp.bfloat16),
            pltpu.VMEM((full, residual.shape[1]), jnp.bfloat16),
            pltpu.VMEM(residual.shape, jnp.float32),
            dma((2,)),
            wide, wide, wide, pltpu.VMEM((span, heads, rows), jnp.float32), wide,
            dma((4, span)), dma((4, span)), dma((span,)), dma((span,)), dma((spread,)), dma((spread,)),
        ],
        compiler_params=pltpu.CompilerParams(
            collective_id=0, has_side_effects=True, vmem_limit_bytes=50 * 1024 * 1024
        ),
        name="mix",
    )(queries, keys, values, g, out_weight, facts, residual, gains)


def experts_kernel(
    span, chunks,
    routed, pick, weigh, gate_in, up_in, down_in, out,
    w_gate, w_up, w_down, mir, out_own, out_mir, arrived, act, res, back, pbuf, part,
    w_sem, mir_s, mir_r, dir_s, dir_r, two_s, two_r, ret_s, ret_r, rt1_s, rt1_r, part_s, part_r,
):
    half = span // 2
    me = lax.axis_index("sp")
    base = (me // half) * half
    loc = me - base
    mirror = lax.rem(me + half, span)
    cap = arrived.shape[2]
    model = routed.shape[1]
    piece = model // chunks
    ff = act.shape[1]
    partners = [(d, lax.rem(loc + d, half)) for d in range(1, half)]
    barrier = pltpu.get_barrier_semaphore()
    for _, p in partners:
        pl.semaphore_signal(barrier, inc=1, device_id={"sp": base + p}, device_id_type=MESH)
    pl.semaphore_signal(barrier, inc=1, device_id={"sp": mirror}, device_id_type=MESH)
    pl.semaphore_wait(barrier, half)

    def remote(src, dst, s_sem, r_sem, device):
        return pltpu.make_async_remote_copy(
            src_ref=src, dst_ref=dst, send_sem=s_sem, recv_sem=r_sem,
            device_id={"sp": device}, device_id_type=MESH,
        )

    def cols(c):
        return pl.ds(c * piece, piece)

    pending = []

    def begin(copy):
        copy.start()
        pending.append(copy)

    edge = is_edge(me, loc, half)
    to_mirror = [
        remote(routed.at[:, cols(c)], mir.at[:, cols(c)], mir_s.at[c], mir_r.at[c], mirror)
        for c in range(chunks)
    ]
    pending.extend(to_mirror)

    @pl.when(jnp.logical_not(edge))
    def _():
        for copy in to_mirror:
            copy.start()

    loads = [
        pltpu.make_async_copy(src, dst, w_sem.at[i])
        for i, (src, dst) in enumerate(((gate_in, w_gate), (up_in, w_up), (down_in, w_down)))
    ]
    for load in loads:
        load.start()

    def rows_of(p):
        return pl.ds(pl.multiple_of(p * cap, cap), cap)

    for d, p in partners:
        chosen = pick[0, rows_of(p), :]
        for c in range(chunks):
            out_own[p, :, cols(c)] = jnp.dot(
                chosen, routed[:, cols(c)], preferred_element_type=jnp.float32
            ).astype(jnp.bfloat16)
        begin(remote(out_own.at[p], arrived.at[0, loc], dir_s.at[d], dir_r.at[loc], base + p))

    @pl.when(edge)
    def _():
        for copy in to_mirror:
            copy.start()

    chosen = pick[0, rows_of(loc), :]
    for c in range(chunks):
        arrived[0, loc, :, cols(c)] = jnp.dot(
            chosen, routed[:, cols(c)], preferred_element_type=jnp.float32
        ).astype(jnp.bfloat16)

    for c in range(chunks):
        remote(mir.at[:, cols(c)], mir.at[:, cols(c)], mir_s.at[c], mir_r.at[c], mirror).wait_recv()
        for d, p in partners:
            out_mir[p, :, cols(c)] = jnp.dot(
                pick[1, rows_of(p), :], mir[:, cols(c)], preferred_element_type=jnp.float32
            ).astype(jnp.bfloat16)
            begin(
                remote(
                    out_mir.at[p, :, cols(c)], arrived.at[1, loc, :, cols(c)],
                    two_s.at[d, c], two_r.at[loc, c], base + p,
                )
            )
        arrived[1, loc, :, cols(c)] = jnp.dot(
            pick[1, rows_of(loc), :], mir[:, cols(c)], preferred_element_type=jnp.float32
        ).astype(jnp.bfloat16)

    for load in loads:
        load.wait()

    def hidden_units(g):
        tile = math.gcd(256, ff)
        rows_in = arrived.at[g]

        def step(f, carry):
            at = pl.ds(pl.multiple_of(f * tile, tile), tile)
            data = rows_in[...].reshape(half * cap, model)
            gate = jnp.dot(data, w_gate[:, at], preferred_element_type=jnp.float32)
            upper = jnp.dot(data, w_up[:, at], preferred_element_type=jnp.float32)
            act[:, at] = (gate / (1.0 + jnp.exp(-gate)) * upper).astype(jnp.bfloat16)
            return carry

        lax.fori_loop(0, ff // tile, step, 0)

    def results(g, c):
        value = jnp.dot(act[...], w_down[:, cols(c)], preferred_element_type=jnp.float32)
        res[g, :, :, cols(c)] = value.astype(jnp.bfloat16).reshape(half, cap, piece)

    def total(g, c):
        data = back[g, :, :, cols(c)].reshape(half * cap, piece)
        high = jnp.dot(weigh[g, 0], data, preferred_element_type=jnp.float32)
        return high + jnp.dot(weigh[g, 1], data, preferred_element_type=jnp.float32)

    for d, p in partners:
        remote(out_own.at[p], arrived.at[0, p], dir_s.at[d], dir_r.at[p], base + p).wait_recv()
    hidden_units(0)
    for c in range(chunks):
        results(0, c)
    for d, p in partners:
        begin(remote(res.at[0, p], back.at[0, loc], ret_s.at[d], ret_r.at[loc], base + p))
    back[0, loc] = res[0, loc]

    for c in range(chunks):
        for d, p in partners:
            remote(
                out_mir.at[p, :, cols(c)], arrived.at[1, p, :, cols(c)],
                two_s.at[d, c], two_r.at[p, c], base + p,
            ).wait_recv()
    hidden_units(1)
    for c in range(chunks):
        results(1, c)
        for d, p in partners:
            begin(
                remote(
                    res.at[1, p, :, cols(c)], back.at[1, loc, :, cols(c)],
                    rt1_s.at[d, c], rt1_r.at[loc, c], base + p,
                )
            )
        back[1, loc, :, cols(c)] = res[1, loc, :, cols(c)]
    for c in range(chunks):
        for d, p in partners:
            remote(
                res.at[1, p, :, cols(c)], back.at[1, p, :, cols(c)],
                rt1_s.at[d, c], rt1_r.at[p, c], base + p,
            ).wait_recv()
        pbuf[:, cols(c)] = total(1, c).astype(jnp.bfloat16)
        begin(remote(pbuf.at[:, cols(c)], part.at[:, cols(c)], part_s.at[c], part_r.at[c], mirror))
    for d, p in partners:
        remote(res.at[0, p], back.at[0, p], ret_s.at[d], ret_r.at[p], base + p).wait_recv()
    for c in range(chunks):
        own = total(0, c)
        remote(pbuf.at[:, cols(c)], part.at[:, cols(c)], part_s.at[c], part_r.at[c], mirror).wait_recv()
        out[:, cols(c)] = own + part[:, cols(c)].astype(jnp.float32)
    for copy in pending:
        copy.wait_send()


def run_experts(routed, pick, weigh, gate_proj, up_proj, down_proj, span, cap):
    rows, model = routed.shape
    ff = gate_proj.shape[1]
    half = span // 2
    chunks = 4 if model % 512 == 0 else 1
    vm = pl.BlockSpec(memory_space=pltpu.VMEM)
    hbm = pl.BlockSpec(memory_space=pl.ANY)
    dma = pltpu.SemaphoreType.DMA
    bf16 = jnp.bfloat16
    return pl.pallas_call(
        functools.partial(experts_kernel, span, chunks),
        out_shape=jax.ShapeDtypeStruct((rows, model), jnp.float32),
        in_specs=[vm, vm, vm, hbm, hbm, hbm],
        out_specs=vm,
        scratch_shapes=[
            pltpu.VMEM((model, ff), bf16), pltpu.VMEM((model, ff), bf16), pltpu.VMEM((ff, model), bf16),
            pltpu.VMEM((rows, model), bf16),
            pltpu.VMEM((half, cap, model), bf16), pltpu.VMEM((half, cap, model), bf16),
            pltpu.VMEM((2, half, cap, model), bf16),
            pltpu.VMEM((half * cap, ff), bf16),
            pltpu.VMEM((2, half, cap, model), bf16), pltpu.VMEM((2, half, cap, model), bf16),
            pltpu.VMEM((rows, model), bf16), pltpu.VMEM((rows, model), bf16),
            dma((3,)), dma((chunks,)), dma((chunks,)), dma((half,)), dma((half,)),
            dma((half, chunks)), dma((half, chunks)), dma((half,)), dma((half,)),
            dma((half, chunks)), dma((half, chunks)), dma((chunks,)), dma((chunks,)),
        ],
        compiler_params=pltpu.CompilerParams(
            collective_id=1, has_side_effects=True, vmem_limit_bytes=58 * 1024 * 1024
        ),
        name="experts",
    )(routed, pick, weigh, gate_proj, up_proj, down_proj)


def body(
    residual, queries, key_vectors, value_vectors, gate_cache, out_weight, mix_gain, route_gain,
    out_gain, routes, group_share, expert_share, gate_proj, up_proj, down_proj,
):
    span = lax.axis_size("sp")
    spread = lax.axis_size("dp")
    tok_rows = residual.shape[1]
    width = queries.shape[2] // span

    top_count = routes.shape[2]
    cap = 4 * tok_rows // span
    half = span // 2
    assigned = routes[0].reshape(-1)
    order = jnp.arange(assigned.shape[0], dtype=jnp.int32)
    same = (assigned[:, None] == assigned[None, :]) & (order[None, :] < order[:, None])
    ranking = jnp.sum(same.astype(jnp.int32), axis=1)
    slots = (assigned * cap + ranking).reshape(routes.shape[1:]).astype(jnp.float32)
    shares = expert_share[0]
    weights = group_share[0][:, None] * shares / jnp.sum(shares, axis=1, keepdims=True)
    facts = jnp.concatenate([slots.T, weights.T], axis=0)
    if width % 128 == 0:
        hidden, routed, other = mix(
            queries[0], key_vectors[0], value_vectors[0], gate_cache[0], out_weight, facts,
            residual[0], jnp.stack([mix_gain, route_gain]), span, spread,
        )
    else:
        by_heads = [
            lax.all_to_all(x, "sp", split_axis=2, concat_axis=1, tiled=True)
            for x in (queries, key_vectors, value_vectors, gate_cache)
        ]
        attended = attend(*(x[0] for x in by_heads))
        by_tokens = lax.all_to_all(attended[None], "sp", split_axis=1, concat_axis=2, tiled=True)[0]
        weight_all = lax.all_gather(out_weight, "dp", axis=1, tiled=True)
        mixed = jnp.dot(by_tokens, weight_all, preferred_element_type=jnp.float32)
        hidden = residual[0].astype(jnp.float32) + normalize(mixed) * mix_gain
        hidden = hidden.astype(jnp.bfloat16)
        routed = (normalize(hidden.astype(jnp.float32)) * route_gain).astype(jnp.bfloat16)
        other = lax.ppermute(facts, "sp", [(i, (i + half) % span) for i in range(span)])
    base = (lax.axis_index("sp") // half) * half
    places = (base * cap + jnp.arange(half * cap, dtype=jnp.int32)).astype(jnp.float32)
    picks, weighs = [], []
    for both in (facts, other):
        slot, share = both[:top_count], both[top_count:]
        picks.append(jnp.any(slot[:, None, :] == places[None, :, None], axis=0).astype(jnp.bfloat16))
        hit = slot[:, :, None] == places[None, None, :]
        high = lax.reduce_precision(share, 8, 7)
        weighs.append(
            jnp.stack(
                [jnp.sum(jnp.where(hit, w[:, :, None], 0.0), axis=0) for w in (high, share - high)]
            ).astype(jnp.bfloat16)
        )
    pick, weigh = jnp.stack(picks), jnp.stack(weighs)

    combined = run_experts(routed, pick, weigh, gate_proj[0], up_proj[0], down_proj[0], span, cap)
    layer_out = (hidden.astype(jnp.float32) + combined * out_gain).astype(jnp.bfloat16)
    return layer_out[None]


def solution(mesh):
    placed = (
        P("dp", "sp", None),
        P("dp", "sp", None),
        P("dp", "sp", None),
        P("dp", "sp", None),
        P("dp", "sp", None),
        P(None, "dp"),
        P(),
        P(),
        P(),
        P("dp", "sp", None),
        P("dp", "sp"),
        P("dp", "sp", None),
        P("sp", None, None),
        P("sp", None, None),
        P("sp", None, None),
    )
    return jax.shard_map(
        body, mesh=mesh, in_specs=placed, out_specs=P("dp", "sp", None), check_vma=False
    )
```
